32 devices in a mesh: grp: 2 (over x), ep: 8 (over z, y), tp: 2 (over core).
Axes of the slice: x: 2, y: 2, z: 4, core: 2. Of those that a mesh axis runs over, the one named last changes fastest.
Arguments:
- tokens: bfloat16 [4096, 2048], P(('grp', 'ep', 'tp')), parts along dimension 0, may hold values from -6 to 6
- expert_ids: int32 [4096, 4], P(('grp', 'ep', 'tp')), parts along dimension 0, may hold values from 0 to 15, all different within a row; in each aligned block of 128 rows (0 to 127, 128 to 255, ...) at most 64 rows name the same one
- route_weights: float32 [4096, 4], P(('grp', 'ep', 'tp')), parts along dimension 0, may hold values from 0.05 to 1
- norm_gain: float32 [2048], replicated, may hold values from 0.1 to 1.9
- w_gate: bfloat16 [16, 2048, 896], P(('ep', 'tp')), may hold values from -0.5 to 0.5
- w_up: bfloat16 [16, 2048, 896], P(('ep', 'tp')), may hold values from -0.5 to 0.5
- w_down: bfloat16 [16, 896, 2048], P(('ep', 'tp')), may hold values from -0.0234375 to 0.0234375
Outputs:
- mixed: bfloat16 [4096, 2048], P(('grp', 'ep', 'tp')), parts along dimension 0
The draws below stay inside these ranges and needn't reach their ends.
There are 2 independent parts, one for each index of `grp`. The reference program is written for one: setup_inputs(seed, part) draws one part's arguments, and reference() takes and returns one part's arrays. A program takes and returns all parts, laid end to end along the dimension named above; an argument that names none is the same for every part. Nothing has to cross between parts.
Inputs may be any that keep to these rules, and one draw needn't show every extreme that they name: `expert_ids`: each token names 4 different experts. Among the 128 tokens of one device (aligned blocks of rows) no expert is named more than 64 times, a bound that some block reaches.
All inputs are finite; a program needn't handle non-finite values.
Results may differ from the reference program's by a relative error of at most 0.0071.
Values may be sent and summed in bfloat16 or wider, within the bound.
No kernel may reach another device: no remote copies, remote signals or barrier semaphores. Data moves between devices by JAX's collectives and lax.ppermute only.
A program may use at most 64 MiB of HBM per device.

```python
import math
import jax
import jax.numpy as jnp
import numpy as np
from jax import lax

D = 2048
F = 896
TOPK = 4
TOK_DEV = 128
EXPERTS = 16
CAP = 64
TOKENS = 2048
N_EP = 8
N_TP = 2


def level_of(key, dims, cuts, smallest, high):
    factor_of = 1.0
    for dim, blocks in cuts:
        draws = jax.random.uniform(jax.random.fold_in(jax.random.fold_in(key, 6), dim), (blocks,), jnp.float32, smallest / len(cuts), high / len(cuts))
        factor_of = factor_of * jnp.repeat(jnp.exp(draws), dims[dim] // blocks).reshape((-1,) + (1,) * (len(dims) - 1 - dim))
    return factor_of


def shared_out(own_key, own, number, rows, amount, top, bound, slope):
    ranking = jax.random.permutation(own_key, amount)
    crowded, common = load_shares(amount, rows * top, bound, slope, True), load_shares(amount, rows * top, bound, slope, False)
    places = jnp.arange(amount)

    def named(sizes, turn):
        used = int((sizes > 0).sum())
        fixed = max(1, used // 4)
        shifted = fixed + (places - fixed + turn * (used - fixed)) % max(1, amount - fixed)
        return jnp.zeros((amount,), jnp.int32).at[ranking[jnp.where(places < fixed, places, shifted)]].set(jnp.asarray(sizes, jnp.int32))

    sizes = jnp.where(number % 4 == 0, named(crowded, number // 4), named(common, number - number // 4 - 1))
    mixed = jax.random.permutation(jax.random.fold_in(own, 3), amount)
    source_of, receiver = mixed[0:amount // 2 * 2:2], mixed[1:amount // 2 * 2:2]
    room = jnp.minimum(sizes[source_of] - 1, bound - sizes[receiver]) // 2
    room = jnp.where((source_of == ranking[0]) | (receiver == ranking[0]) | (sizes[receiver] == 0), 0, jnp.maximum(room, 0))
    shifted = jax.random.randint(jax.random.fold_in(own, 4), (amount // 2,), 0, 1 << 20) % (room + 1)
    sizes = sizes.at[source_of].add(-shifted).at[receiver].add(shifted)
    items = jnp.searchsorted(jnp.cumsum(sizes), jnp.arange(rows * top), side="right").astype(jnp.int32)
    grid = items.reshape(top, rows).T
    grid = grid[jax.random.permutation(jax.random.fold_in(own, 1), rows)]
    turn = jax.random.randint(jax.random.fold_in(own, 2), (rows, 1), 0, top)
    return jnp.take_along_axis(grid, (jnp.arange(top)[None, :] + turn) % top, axis=1)


def load_shares(amount, total, limit, lean, full):
    loads = [(1 << 20) // math.isqrt(standing ** lean) + 1 for standing in range(1, amount + 1)]
    largest = limit if full else min(limit, max(-(-total // amount), total * loads[0] // sum(loads)))
    least = 1 if total - largest >= amount - 1 else 0
    given, surplus = [largest] + [least] * (amount - 1), total - largest - least * (amount - 1)
    while surplus > 0:
        free = [i for i in range(1, amount) if given[i] < largest] or [i for i in range(1, amount) if given[i] < limit]
        whole, left = sum([loads[i] for i in free]), surplus
        for i in free:
            extra = min(limit - given[i], max(1, left * loads[i] // whole), surplus)
            given[i] = given[i] + extra
            surplus = surplus - extra
    return np.array(given)


def noise(stream_key, shape, scale, limit, cuts=(), kind=jnp.bfloat16):
    gain = level_of(stream_key, shape, cuts, -0.22, 0.18) if cuts else 1.0
    values = jax.random.normal(stream_key, shape, jnp.float32) * scale * gain
    return jnp.minimum(jnp.maximum(values, -limit), limit).astype(kind)


def setup_inputs(seed: int = 0, part: int = 0) -> dict:
    splits = jax.random.split(jax.random.key(seed), 8)
    part_splits = jax.random.split(jax.random.fold_in(splits[7], part), 8)
    tokens = noise(part_splits[0], (TOKENS, D), 1.0, 6.0, ((0, 16),))
    expert_ids_keys = jax.random.split(jax.random.fold_in(part_splits[1], 1), TOKENS // TOK_DEV)
    expert_ids_turns = jax.random.permutation(jax.random.fold_in(part_splits[1], 3), TOKENS // TOK_DEV)
    expert_ids = jax.vmap(lambda own, number: shared_out(jax.random.fold_in(part_splits[1], 2), own, number, TOK_DEV, EXPERTS, TOPK, CAP, 2))(expert_ids_keys, expert_ids_turns).reshape((TOKENS, TOPK))
    route_weights = jnp.clip(jnp.exp(math.log(1.0) - 2.9957323 * jax.random.uniform(part_splits[2], (TOKENS, TOPK), jnp.float32) ** level_of(part_splits[2], (TOKENS, TOPK), ((0, 16),), -0.2, 0.2)), 0.05, 1.0)
    norm_gain = jnp.clip(1.0 + 0.18 * jax.random.normal(splits[3], (D,), jnp.float32), 0.1, 1.9)
    w_gate = noise(splits[4], (EXPERTS, D, F), (D // 16) ** -0.5, 0.5, ((0, 16),))
    w_up = noise(splits[5], (EXPERTS, D, F), (D // 16) ** -0.5, 0.5, ((0, 16),))
    w_down = noise(splits[6], (EXPERTS, F, D), (64 * F) ** -0.5, 0.0234375, ((0, 16),))
    return {"tokens": tokens, "expert_ids": expert_ids, "route_weights": route_weights, "norm_gain": norm_gain, "w_gate": w_gate, "w_up": w_up, "w_down": w_down}


norm_eps = 1e-05
clamp_limit = 7.0
sig_alpha = 1.702

def layer_norm(tokens, norm_gain):
    values = tokens.astype(jnp.float32)
    row_mean = lax.optimization_barrier(jnp.mean(values, -1, keepdims=True))
    centred = values - row_mean
    row_var = lax.optimization_barrier(jnp.mean(centred * centred, -1, keepdims=True))
    scaled = centred * lax.rsqrt(row_var + norm_eps) * norm_gain.astype(jnp.float32)
    return scaled.astype(jnp.bfloat16)

def expert_apply(inputs, gate_mat, up_mat, down_mat):
    gate_pre = jnp.dot(inputs, gate_mat, preferred_element_type=jnp.float32)
    up_pre = jnp.dot(inputs, up_mat, preferred_element_type=jnp.float32)
    gated = jnp.minimum(gate_pre, clamp_limit)
    upper = jnp.clip(up_pre, -clamp_limit, clamp_limit)
    hidden = (gated * jax.nn.sigmoid(sig_alpha * gated) * (upper + 1.0)).astype(jnp.bfloat16)
    return jnp.dot(hidden, down_mat, preferred_element_type=jnp.float32).astype(jnp.bfloat16)

def reference(tokens, expert_ids, route_weights, norm_gain, w_gate, w_up, w_down):
    normed = layer_norm(tokens, norm_gain)
    flat_ids = expert_ids.reshape(-1).astype(jnp.int32)
    sorted_pairs = jnp.argsort(flat_ids, stable=True).astype(jnp.int32)
    counts = lax.optimization_barrier(jnp.sum((flat_ids[:, None] == jnp.arange(EXPERTS, dtype=jnp.int32)[None, :]).astype(jnp.int32), 0))
    starts = (jnp.cumsum(counts) - counts).astype(jnp.int32)
    slot_limit = N_EP * N_TP * CAP
    padded = jnp.concatenate([sorted_pairs, jnp.zeros((slot_limit,), jnp.int32)])
    pair_weights = route_weights.reshape(-1).astype(jnp.float32)

    def add_expert(accum_total, inputs):
        expert, gate_mat, up_mat, down_mat = inputs
        pair_index = lax.dynamic_slice_in_dim(padded, starts[expert].astype(jnp.int32), slot_limit)
        live_mask = jnp.arange(slot_limit, dtype=jnp.int32) < counts[expert]
        token_index = (pair_index // TOPK).astype(jnp.int32)
        results = expert_apply(normed[token_index], gate_mat, up_mat, down_mat)
        factor = jnp.where(live_mask, pair_weights[pair_index], jnp.zeros((), jnp.float32))
        scaled = factor[:, None] * results.astype(jnp.float32)
        return (accum_total.at[token_index].add(scaled), None)
    start_total = jnp.zeros((TOKENS, D), jnp.float32)
    accum_total, unused = lax.scan(add_expert, start_total, (jnp.arange(EXPERTS, dtype=jnp.int32), w_gate, w_up, w_down))
    return accum_total.astype(jnp.bfloat16)
```

```python
import jax
import jax.numpy as jnp
from jax import lax
from jax.sharding import PartitionSpec as P

norm_eps = 1e-05
clamp_limit = 7.0
sig_alpha = 1.702


def layer_norm(tokens, norm_gain):
    values = tokens.astype(jnp.float32)
    row_mean = jnp.mean(values, -1, keepdims=True)
    centred = values - row_mean
    row_var = jnp.mean(centred * centred, -1, keepdims=True)
    scaled = centred * lax.rsqrt(row_var + norm_eps) * norm_gain
    return scaled.astype(jnp.bfloat16)


def expert_apply(inputs, gate_mat, up_mat, down_mat):
    gate_pre = jnp.dot(inputs, gate_mat, preferred_element_type=jnp.float32)
    up_pre = jnp.dot(inputs, up_mat, preferred_element_type=jnp.float32)
    gated = jnp.minimum(gate_pre, clamp_limit)
    upper = jnp.clip(up_pre, -clamp_limit, clamp_limit)
    hidden = (gated * jax.nn.sigmoid(sig_alpha * gated) * (upper + 1.0)).astype(jnp.bfloat16)
    return jnp.dot(hidden, down_mat, preferred_element_type=jnp.float32).astype(jnp.bfloat16)


def local(tokens, expert_ids, route_weights, norm_gain, w_gate, w_up, w_down):
    ep_count = lax.axis_size("ep")
    tp_count = lax.axis_size("tp")
    experts = ep_count * tp_count
    tok_rows, feat_width = tokens.shape
    top_count = expert_ids.shape[1]
    capacity = 2 * tok_rows * top_count // experts
    normed = layer_norm(tokens, norm_gain)
    flat_ids = expert_ids.reshape(-1)
    one_hot = (flat_ids[:, None] == jnp.arange(experts, dtype=jnp.int32)[None, :]).astype(jnp.int32)
    slot_index = jnp.sum((jnp.cumsum(one_hot, 0) - one_hot) * one_hot, 1)
    target = flat_ids * capacity + slot_index
    pair_token = jnp.arange(tok_rows * top_count, dtype=jnp.int32) // top_count
    buffer = (
        jnp.zeros((experts * capacity, feat_width), jnp.bfloat16).at[target].set(normed[pair_token])
    )
    buffer = buffer.reshape(experts, capacity, feat_width)
    gate_mat = w_gate[0]
    up_mat = w_up[0]
    down_mat = w_down[0]
    arrived = lax.all_to_all(buffer, ("ep", "tp"), split_axis=0, concat_axis=0, tiled=True)
    flat_rows = arrived.reshape(-1, feat_width)
    returned = lax.all_to_all(
        expert_apply(flat_rows, gate_mat, up_mat, down_mat).reshape(arrived.shape),
        ("ep", "tp"),
        split_axis=0,
        concat_axis=0,
        tiled=True,
    )
    picked = returned.reshape(experts * capacity, feat_width)[target].reshape(
        tok_rows, top_count, feat_width
    )
    combined = jnp.zeros((tok_rows, feat_width), jnp.float32)
    for choice_slot in range(top_count):
        combined = combined + route_weights[:, choice_slot : choice_slot + 1] * picked[
            :, choice_slot
        ].astype(jnp.float32)
    return combined.astype(jnp.bfloat16)


def dense_weights(expert_ids, route_weights, experts):
    chosen = expert_ids[None, :, :] == jnp.arange(experts, dtype=jnp.int32)[:, None, None]
    return jnp.sum(jnp.where(chosen, route_weights[None, :, :], 0.0), -1)


def expert_weighted(inputs, scale, gate_mat, up_mat, down_mat):
    gate_pre = jnp.dot(inputs, gate_mat, preferred_element_type=jnp.float32)
    up_pre = jnp.dot(inputs, up_mat, preferred_element_type=jnp.float32)
    gated = jnp.minimum(gate_pre, clamp_limit)
    upper = jnp.clip(up_pre, -clamp_limit, clamp_limit)
    hidden = (gated * jax.nn.sigmoid(sig_alpha * gated) * (upper + 1.0)).astype(jnp.bfloat16)
    out = jnp.dot(hidden, down_mat, preferred_element_type=jnp.float32)
    return (out * scale[:, None]).astype(jnp.bfloat16)


def ring_local(tokens, expert_ids, route_weights, norm_gain, w_gate, w_up, w_down):
    ep_count = lax.axis_size("ep")
    tp_count = lax.axis_size("tp")
    tok_rows, feat_width = tokens.shape
    half = ep_count // 2
    order = list(range(0, ep_count, 2)) + list(range(ep_count - 1, 0, -2))
    ahead = [(order[i], order[(i + 1) % ep_count]) for i in range(ep_count)]
    behind = [(b, a) for a, b in ahead]
    swap = [(0, 1), (1, 0)]
    pieces = 2
    rows = tok_rows // pieces
    normed = layer_norm(tokens, norm_gain)
    start = [normed[c * rows : (c + 1) * rows] for c in range(pieces)]

    def shift(value, pairs):
        return lax.ppermute(value, "ep", pairs)

    def other(value):
        return lax.ppermute(value, "tp", swap)

    held = [[{} for _ in range(half + 1)] for _ in range(2)]
    for direction in range(2):
        held[direction][0] = {c: start[c] for c in range(pieces)}
    for step in range(1, half + 1):
        for c in range(pieces):
            for direction, pairs in ((0, ahead), (1, behind)):
                if step == half and c % 2 != direction:
                    continue
                held[direction][step][c] = shift(held[direction][step - 1][c], pairs)

    weights = dense_weights(expert_ids, route_weights, ep_count * tp_count)
    weights = lax.all_to_all(weights, ("ep", "tp"), split_axis=0, concat_axis=0, tiled=True)
    place = jnp.asarray([order.index(i) for i in range(ep_count)], jnp.int32)[lax.axis_index("ep")]
    back = lax.rem(place + ep_count - jnp.arange(ep_count, dtype=jnp.int32), ep_count)
    owner = jnp.asarray(order, jnp.int32)[back]
    side = lax.axis_index("tp")
    lines = jnp.stack([owner * tp_count + side, owner * tp_count + (1 - side)], 1).reshape(-1)
    weights = weights[lines].reshape(ep_count, tp_count, pieces, rows)

    def scale_of(direction, step, whose, c):
        return weights[(step if direction == 0 else ep_count - step) % ep_count, whose, c]

    sums = [[{} for _ in range(half + 1)] for _ in range(2)]
    for step in list(range(0, half + 1)):
        keys = []
        for direction in range(2):
            if step == 0 and direction == 1:
                continue
            keys += [(direction, c) for c in sorted(held[direction][step])]
        mine = [held[d][step][c] for d, c in keys]
        theirs = [other(v) for v in mine]
        block = jnp.concatenate(mine + theirs, 0)
        scale = jnp.concatenate(
            [scale_of(d, step, 0, c) for d, c in keys] + [scale_of(d, step, 1, c) for d, c in keys]
        )
        result = expert_weighted(block, scale, w_gate[0], w_up[0], w_down[0])
        count = len(keys)
        for i, (d, c) in enumerate(keys):
            own = result[i * rows : (i + 1) * rows]
            from_other = other(result[(count + i) * rows : (count + i + 1) * rows])
            sums[d][step][c] = own.astype(jnp.float32) + from_other.astype(jnp.float32)

    arrived = [{}, {}]
    for step in range(half, 0, -1):
        for c in range(pieces):
            for direction, pairs in ((0, behind), (1, ahead)):
                if c not in sums[direction][step]:
                    continue
                total = sums[direction][step][c]
                if c in arrived[direction]:
                    total = total + arrived[direction][c].astype(jnp.float32)
                arrived[direction][c] = shift(total.astype(jnp.bfloat16), pairs)
    done = [
        (sums[0][0][c] + arrived[0][c].astype(jnp.float32) + arrived[1][c].astype(jnp.float32)).astype(
            jnp.bfloat16
        )
        for c in range(pieces)
    ]
    return jnp.concatenate(done, 0)


def solution(mesh):
    placed = (
        P(("grp", "ep", "tp"), None),
        P(("grp", "ep", "tp"), None),
        P(("grp", "ep", "tp"), None),
        P(),
        P(("ep", "tp"), None, None),
        P(("ep", "tp"), None, None),
        P(("ep", "tp"), None, None),
    )

    def body(tokens, expert_ids, *rest):
        experts = mesh.shape["ep"] * mesh.shape["tp"]
        tok_rows = tokens.shape[0]
        capacity = 2 * tok_rows * expert_ids.shape[1] // experts
        ring = 2 * capacity >= tok_rows and mesh.shape["ep"] % 2 == 0 and mesh.shape["tp"] == 2
        return (ring_local if ring else local)(tokens, expert_ids, *rest)

    return jax.shard_map(
        body, mesh=mesh, in_specs=placed, out_specs=P(("grp", "ep", "tp"), None), check_vma=False
    )
```

```python
import functools

import jax
import jax.numpy as jnp
from jax import lax
from jax.experimental import pallas as pl
from jax.experimental.pallas import tpu as pltpu
from jax.sharding import PartitionSpec as P

norm_eps = 1e-05
clamp_limit = 7.0
sig_alpha = 1.702


def layer_norm(tokens, norm_gain):
    values = tokens.astype(jnp.float32)
    row_mean = jnp.mean(values, -1, keepdims=True)
    centred = values - row_mean
    row_var = jnp.mean(centred * centred, -1, keepdims=True)
    scaled = centred * lax.rsqrt(row_var + norm_eps) * norm_gain
    return scaled.astype(jnp.bfloat16)


def expert_apply(inputs, gate_mat, up_mat, down_mat):
    gate_pre = jnp.dot(inputs, gate_mat, preferred_element_type=jnp.float32)
    up_pre = jnp.dot(inputs, up_mat, preferred_element_type=jnp.float32)
    gated = jnp.minimum(gate_pre, clamp_limit)
    upper = jnp.clip(up_pre, -clamp_limit, clamp_limit)
    hidden = (gated * jax.nn.sigmoid(sig_alpha * gated) * (upper + 1.0)).astype(jnp.bfloat16)
    return jnp.dot(hidden, down_mat, preferred_element_type=jnp.float32).astype(jnp.bfloat16)


def local(tokens, expert_ids, route_weights, norm_gain, w_gate, w_up, w_down):
    ep_count = lax.axis_size("ep")
    tp_count = lax.axis_size("tp")
    experts = ep_count * tp_count
    tok_rows, feat_width = tokens.shape
    top_count = expert_ids.shape[1]
    capacity = 2 * tok_rows * top_count // experts
    normed = layer_norm(tokens, norm_gain)
    flat_ids = expert_ids.reshape(-1)
    one_hot = (flat_ids[:, None] == jnp.arange(experts, dtype=jnp.int32)[None, :]).astype(jnp.int32)
    slot_index = jnp.sum((jnp.cumsum(one_hot, 0) - one_hot) * one_hot, 1)
    target = flat_ids * capacity + slot_index
    pair_token = jnp.arange(tok_rows * top_count, dtype=jnp.int32) // top_count
    buffer = (
        jnp.zeros((experts * capacity, feat_width), jnp.bfloat16).at[target].set(normed[pair_token])
    )
    buffer = buffer.reshape(experts, capacity, feat_width)
    gate_mat = w_gate[0]
    up_mat = w_up[0]
    down_mat = w_down[0]
    arrived = lax.all_to_all(buffer, ("ep", "tp"), split_axis=0, concat_axis=0, tiled=True)
    flat_rows = arrived.reshape(-1, feat_width)
    returned = lax.all_to_all(
        expert_apply(flat_rows, gate_mat, up_mat, down_mat).reshape(arrived.shape),
        ("ep", "tp"),
        split_axis=0,
        concat_axis=0,
        tiled=True,
    )
    picked = returned.reshape(experts * capacity, feat_width)[target].reshape(
        tok_rows, top_count, feat_width
    )
    combined = jnp.zeros((tok_rows, feat_width), jnp.float32)
    for choice_slot in range(top_count):
        combined = combined + route_weights[:, choice_slot : choice_slot + 1] * picked[
            :, choice_slot
        ].astype(jnp.float32)
    return combined.astype(jnp.bfloat16)


def expert_kernel(tok_rows, capacity, experts, pieces, pairs, *refs):
    number = pairs * 2 * pieces
    which = refs[0]
    blocks = refs[1 : 1 + number]
    gate_hbm, up_hbm, down_hbm, own_out, other_out = refs[1 + number : 6 + number]
    gate_mat, up_mat, down_mat, chosen, hidden, weight, spread, sems = refs[6 + number :]
    feat_width, hid_width = gate_mat.shape
    tile = 256
    hid_tiles, out_tiles = hid_width // tile, feat_width // tile
    tail = hid_width - hid_tiles * tile

    def hid_copy(i, at, width):
        cols = pl.ds(at, width)
        return (
            pltpu.make_async_copy(gate_hbm.at[0, :, cols], gate_mat.at[:, cols], sems.at[0, i]),
            pltpu.make_async_copy(up_hbm.at[0, :, cols], up_mat.at[:, cols], sems.at[1, i]),
        )

    def out_copy(i, at):
        cols = pl.ds(at, tile)
        return pltpu.make_async_copy(down_hbm.at[0, :, cols], down_mat.at[:, cols], sems.at[2, i])

    for i in range(hid_tiles):
        for copy in hid_copy(i, i * tile, tile):
            copy.start()
    if tail:
        for copy in hid_copy(hid_tiles, hid_tiles * tile, tail):
            copy.start()
    for i in range(out_tiles):
        out_copy(i, i * tile).start()

    tokens, slots = 2 * tok_rows, 2 * capacity
    row = lax.broadcasted_iota(jnp.int32, (tokens, tokens), 0)
    col = lax.broadcasted_iota(jnp.int32, (tokens, tokens), 1)
    earlier = (col < row) & ((col >= tok_rows) == (row >= tok_rows))
    earlier = jnp.where(earlier, 1.0, 0.0).astype(jnp.bfloat16)
    for p in range(pairs):
        mine = blocks[p * 2 * pieces : (p + 1) * 2 * pieces]
        extra = jnp.concatenate([r[:, feat_width:] for r in mine], 0).astype(jnp.float32)
        lane = lax.broadcasted_iota(jnp.int32, extra.shape, 1)
        wanted = (lane == which[0]) | (lane == which[0] + experts)
        scale = jnp.sum(jnp.where(wanted, extra, 0.0), 1, keepdims=True)
        mask = jnp.broadcast_to(jnp.where(scale > 0.0, 1.0, 0.0), (tokens, slots))
        place = jnp.dot(earlier, mask.astype(jnp.bfloat16), preferred_element_type=jnp.float32)
        line = lax.broadcasted_iota(jnp.int32, (tokens, slots), 0)
        slot = lax.broadcasted_iota(jnp.int32, (tokens, slots), 1)
        target = place.astype(jnp.int32) + jnp.where(line >= tok_rows, capacity, 0)
        spread[p] = jnp.where((target == slot) & (mask > 0.0), 1.0, 0.0).astype(jnp.bfloat16)
        weight[p] = jnp.broadcast_to(scale, (tokens, 128))

        @pl.loop(0, feat_width // tile)
        def _(i):
            cols = pl.ds(pl.multiple_of(i * tile, tile), tile)
            part = jnp.concatenate([r[:, cols] for r in mine], 0)
            picked = lax.dot_general(
                spread[p], part, (((0,), (0,)), ((), ())), preferred_element_type=jnp.float32
            )
            chosen[p * slots : (p + 1) * slots, cols] = picked.astype(jnp.bfloat16)

    def hid_tile(i, at, width):
        for copy in hid_copy(i, at, width):
            copy.wait()
        cols = pl.ds(at, width)
        gate_pre = jnp.dot(chosen[...], gate_mat[:, cols], preferred_element_type=jnp.float32)
        up_pre = jnp.dot(chosen[...], up_mat[:, cols], preferred_element_type=jnp.float32)
        gated = jnp.minimum(gate_pre, clamp_limit)
        upper = jnp.clip(up_pre, -clamp_limit, clamp_limit)
        value = gated * jax.nn.sigmoid(sig_alpha * gated) * (upper + 1.0)
        hidden[:, cols] = value.astype(jnp.bfloat16)

    @pl.loop(0, hid_tiles)
    def _(i):
        hid_tile(i, pl.multiple_of(i * tile, tile), tile)

    if tail:
        hid_tile(hid_tiles, hid_tiles * tile, tail)

    @pl.loop(0, out_tiles)
    def _(i):
        at = pl.multiple_of(i * tile, tile)
        out_copy(i, at).wait()
        cols = pl.ds(at, tile)
        out = jnp.dot(hidden[...], down_mat[:, cols], preferred_element_type=jnp.float32)
        out = out.astype(jnp.bfloat16)
        for p in range(pairs):
            full = jnp.dot(
                spread[p], out[p * slots : (p + 1) * slots], preferred_element_type=jnp.float32
            )
            full = (full * weight[p][:, :1]).astype(jnp.bfloat16)
            own_out[p * tok_rows : (p + 1) * tok_rows, cols] = full[:tok_rows]
            other_out[p * tok_rows : (p + 1) * tok_rows, cols] = full[tok_rows:]


def expert_blocks(which, groups, w_gate, w_up, w_down, tok_rows, capacity, experts):
    pairs, pieces = len(groups), len(groups[0]) // 2
    flat = [v for g in groups for v in g]
    feat_width, hid_width = w_gate.shape[1:]
    tokens, slots = 2 * tok_rows, 2 * capacity
    rows = pairs * slots
    shape = jax.ShapeDtypeStruct((pairs * tok_rows, feat_width), jnp.bfloat16)
    vmem = pl.BlockSpec(memory_space=pltpu.VMEM)
    return pl.pallas_call(
        functools.partial(expert_kernel, tok_rows, capacity, experts, pieces, pairs),
        out_shape=(shape, shape),
        in_specs=[pl.BlockSpec(memory_space=pltpu.SMEM)]
        + [vmem] * len(flat)
        + [pl.BlockSpec(memory_space=pl.ANY)] * 3,
        out_specs=(vmem, vmem),
        scratch_shapes=[
            pltpu.VMEM((feat_width, hid_width), jnp.bfloat16),
            pltpu.VMEM((feat_width, hid_width), jnp.bfloat16),
            pltpu.VMEM((hid_width, feat_width), jnp.bfloat16),
            pltpu.VMEM((rows, feat_width), jnp.bfloat16),
            pltpu.VMEM((rows, hid_width), jnp.bfloat16),
            pltpu.VMEM((pairs, tokens, 128), jnp.float32),
            pltpu.VMEM((pairs, tokens, slots), jnp.bfloat16),
            pltpu.SemaphoreType.DMA((3, 8)),
        ],
        compiler_params=pltpu.CompilerParams(vmem_limit_bytes=40 * 2**20),
        cost_estimate=pl.CostEstimate(
            flops=6 * rows * feat_width * hid_width,
            bytes_accessed=6 * feat_width * hid_width,
            transcendentals=rows * hid_width,
        ),
    )(which, *flat, w_gate, w_up, w_down)


def ring_local(tokens, expert_ids, route_weights, norm_gain, w_gate, w_up, w_down):
    ep_count = lax.axis_size("ep")
    tp_count = lax.axis_size("tp")
    experts = ep_count * tp_count
    tok_rows, feat_width = tokens.shape
    capacity = 2 * tok_rows * expert_ids.shape[1] // experts
    half = ep_count // 2
    order = list(range(0, ep_count, 2)) + list(range(ep_count - 1, 0, -2))
    ahead = [(order[i], order[(i + 1) % ep_count]) for i in range(ep_count)]
    behind = [(b, a) for a, b in ahead]
    swap = [(0, 1), (1, 0)]
    pieces = 2
    rows = tok_rows // pieces
    normed = layer_norm(tokens, norm_gain)
    fits = expert_ids[:, :, None] == jnp.arange(experts, dtype=jnp.int32)
    weights = jnp.sum(jnp.where(fits, route_weights[:, :, None], 0.0), 1)
    high = weights.astype(jnp.bfloat16)
    low = (weights - high.astype(jnp.float32)).astype(jnp.bfloat16)
    lanes = -(-2 * experts // 128) * 128
    gap = jnp.zeros((tok_rows, lanes - 2 * experts), jnp.bfloat16)
    packed = jnp.concatenate([normed, high, low, gap], 1)
    start = [packed[c * rows : (c + 1) * rows] for c in range(pieces)]
    which = (lax.axis_index("ep") * tp_count + lax.axis_index("tp")).astype(jnp.int32).reshape(1)

    def shift(value, pairs):
        return lax.ppermute(value, "ep", pairs)

    def other(value):
        return lax.ppermute(value, "tp", swap)

    held = [[{} for _ in range(half + 1)] for _ in range(2)]
    for direction in range(2):
        held[direction][0] = {c: start[c] for c in range(pieces)}
    for step in range(1, half + 1):
        for c in range(pieces):
            for direction, pairs in ((0, ahead), (1, behind)):
                if step == half and c % 2 != direction:
                    continue
                held[direction][step][c] = shift(held[direction][step - 1][c], pairs)

    sums = [[{} for _ in range(half + 1)] for _ in range(2)]
    for step in range(half + 1):
        if step == 0:
            groups = [[(0, c) for c in range(pieces)]]
        elif step == half:
            groups = [[(c % 2, c) for c in range(pieces)]]
        else:
            groups = [[(d, c) for c in range(pieces)] for d in range(2)]
        values = []
        for g in groups:
            mine = [held[d][step][c] for d, c in g]
            values.append(mine + [other(v) for v in mine])
        own, theirs = expert_blocks(
            which, values, w_gate, w_up, w_down, tok_rows, capacity, experts
        )
        returned = other(theirs)
        for i, (d, c) in enumerate([k for g in groups for k in g]):
            part = slice(i * rows, (i + 1) * rows)
            sums[d][step][c] = own[part].astype(jnp.float32) + returned[part].astype(jnp.float32)

    arrived = [{}, {}]
    for step in range(half, 0, -1):
        for c in range(pieces):
            for direction, pairs in ((0, behind), (1, ahead)):
                if c not in sums[direction][step]:
                    continue
                total = sums[direction][step][c]
                if c in arrived[direction]:
                    total = total + arrived[direction][c].astype(jnp.float32)
                arrived[direction][c] = shift(total.astype(jnp.bfloat16), pairs)
    done = [
        (sums[0][0][c] + arrived[0][c].astype(jnp.float32) + arrived[1][c].astype(jnp.float32)).astype(
            jnp.bfloat16
        )
        for c in range(pieces)
    ]
    return jnp.concatenate(done, 0)


def solution(mesh):
    placed = (
        P(("grp", "ep", "tp"), None),
        P(("grp", "ep", "tp"), None),
        P(("grp", "ep", "tp"), None),
        P(),
        P(("ep", "tp"), None, None),
        P(("ep", "tp"), None, None),
        P(("ep", "tp"), None, None),
    )

    def body(tokens, expert_ids, *rest):
        experts = mesh.shape["ep"] * mesh.shape["tp"]
        tok_rows = tokens.shape[0]
        capacity = 2 * tok_rows * expert_ids.shape[1] // experts
        ring = 2 * capacity >= tok_rows and mesh.shape["ep"] % 2 == 0 and mesh.shape["tp"] == 2
        return (ring_local if ring else local)(tokens, expert_ids, *rest)

    return jax.shard_map(
        body, mesh=mesh, in_specs=placed, out_specs=P(("grp", "ep", "tp"), None), check_vma=False
    )
```

```python
import functools

import jax
import jax.numpy as jnp
from jax import lax
from jax.experimental import pallas as pl
from jax.experimental.pallas import tpu as pltpu
from jax.sharding import PartitionSpec as P


norm_eps = 1e-05
clamp_limit = 7.0
sig_alpha = 1.702


def layer_norm(tokens, norm_gain):
    values = tokens.astype(jnp.float32)
    row_mean = jnp.mean(values, -1, keepdims=True)
    centred = values - row_mean
    row_var = jnp.mean(centred * centred, -1, keepdims=True)
    scaled = centred * lax.rsqrt(row_var + norm_eps) * norm_gain
    return scaled.astype(jnp.bfloat16)


def expert_apply(inputs, gate_mat, up_mat, down_mat):
    gate_pre = jnp.dot(inputs, gate_mat, preferred_element_type=jnp.float32)
    up_pre = jnp.dot(inputs, up_mat, preferred_element_type=jnp.float32)
    gated = jnp.minimum(gate_pre, clamp_limit)
    upper = jnp.clip(up_pre, -clamp_limit, clamp_limit)
    hidden = (gated * jax.nn.sigmoid(sig_alpha * gated) * (upper + 1.0)).astype(jnp.bfloat16)
    return jnp.dot(hidden, down_mat, preferred_element_type=jnp.float32).astype(jnp.bfloat16)


def local(tokens, expert_ids, route_weights, norm_gain, w_gate, w_up, w_down):
    ep_count = lax.axis_size("ep")
    tp_count = lax.axis_size("tp")
    experts = ep_count * tp_count
    tok_rows, feat_width = tokens.shape
    top_count = expert_ids.shape[1]
    capacity = 2 * tok_rows * top_count // experts
    normed = layer_norm(tokens, norm_gain)
    flat_ids = expert_ids.reshape(-1)
    one_hot = (flat_ids[:, None] == jnp.arange(experts, dtype=jnp.int32)[None, :]).astype(jnp.int32)
    slot_index = jnp.sum((jnp.cumsum(one_hot, 0) - one_hot) * one_hot, 1)
    target = flat_ids * capacity + slot_index
    pair_token = jnp.arange(tok_rows * top_count, dtype=jnp.int32) // top_count
    buffer = (
        jnp.zeros((experts * capacity, feat_width), jnp.bfloat16).at[target].set(normed[pair_token])
    )
    buffer = buffer.reshape(experts, capacity, feat_width)
    gate_mat = w_gate[0]
    up_mat = w_up[0]
    down_mat = w_down[0]
    arrived = lax.all_to_all(buffer, ("ep", "tp"), split_axis=0, concat_axis=0, tiled=True)
    flat_rows = arrived.reshape(-1, feat_width)
    returned = lax.all_to_all(
        expert_apply(flat_rows, gate_mat, up_mat, down_mat).reshape(arrived.shape),
        ("ep", "tp"),
        split_axis=0,
        concat_axis=0,
        tiled=True,
    )
    picked = returned.reshape(experts * capacity, feat_width)[target].reshape(
        tok_rows, top_count, feat_width
    )
    combined = jnp.zeros((tok_rows, feat_width), jnp.float32)
    for choice_slot in range(top_count):
        combined = combined + route_weights[:, choice_slot : choice_slot + 1] * picked[
            :, choice_slot
        ].astype(jnp.float32)
    return combined.astype(jnp.bfloat16)


def expert_kernel(tok_rows, capacity, experts, pieces, pairs, *refs):
    number = pairs * 2 * pieces
    which = refs[0]
    blocks = refs[1 : 1 + number]
    gate_hbm, up_hbm, down_hbm, own_out, other_out = refs[1 + number : 6 + number]
    gate_mat, up_mat, down_mat, chosen, hidden, weight, spread, gather, sems = refs[6 + number :]
    feat_width, hid_width = gate_mat.shape
    tile = 256
    hid_tiles, out_tiles = hid_width // tile, feat_width // tile
    tail = hid_width - hid_tiles * tile

    def hid_copy(i, at, width):
        cols = pl.ds(at, width)
        return (
            pltpu.make_async_copy(gate_hbm.at[0, :, cols], gate_mat.at[:, cols], sems.at[0, i]),
            pltpu.make_async_copy(up_hbm.at[0, :, cols], up_mat.at[:, cols], sems.at[1, i]),
        )

    def out_copy(i, at):
        cols = pl.ds(at, tile)
        return pltpu.make_async_copy(down_hbm.at[0, :, cols], down_mat.at[:, cols], sems.at[2, i])

    for i in range(hid_tiles):
        for copy in hid_copy(i, i * tile, tile):
            copy.start()
    if tail:
        for copy in hid_copy(hid_tiles, hid_tiles * tile, tail):
            copy.start()
    for i in range(out_tiles):
        out_copy(i, i * tile).start()

    tokens, slots = 2 * tok_rows, 2 * capacity
    row = lax.broadcasted_iota(jnp.int32, (tokens, tokens), 0)
    col = lax.broadcasted_iota(jnp.int32, (tokens, tokens), 1)
    earlier = (col < row) & ((col >= tok_rows) == (row >= tok_rows))
    earlier = jnp.where(earlier, 1.0, 0.0).astype(jnp.bfloat16)
    for p in range(pairs):
        mine = blocks[p * 2 * pieces : (p + 1) * 2 * pieces]
        extra = jnp.concatenate([r[:, feat_width:] for r in mine], 0).astype(jnp.float32)
        lane = lax.broadcasted_iota(jnp.int32, extra.shape, 1)
        wanted = (lane == which[0]) | (lane == which[0] + experts)
        scale = jnp.sum(jnp.where(wanted, extra, 0.0), 1, keepdims=True)
        mask = jnp.broadcast_to(jnp.where(scale > 0.0, 1.0, 0.0), (tokens, slots))
        place = jnp.dot(earlier, mask.astype(jnp.bfloat16), preferred_element_type=jnp.float32)
        line = lax.broadcasted_iota(jnp.int32, (tokens, slots), 0)
        slot = lax.broadcasted_iota(jnp.int32, (tokens, slots), 1)
        target = place.astype(jnp.int32) + jnp.where(line >= tok_rows, capacity, 0)
        one_hot = jnp.where((target == slot) & (mask > 0.0), 1.0, 0.0)
        spread[p] = one_hot.astype(jnp.bfloat16)
        gather[p] = one_hot.T.astype(jnp.bfloat16)
        weight[p] = jnp.broadcast_to(scale, (tokens, tile))

        @pl.loop(0, feat_width // tile)
        def _(i):
            cols = pl.ds(pl.multiple_of(i * tile, tile), tile)
            part = jnp.concatenate([r[:, cols] for r in mine], 0)
            picked = jnp.dot(gather[p], part, preferred_element_type=jnp.float32)
            chosen[p * slots : (p + 1) * slots, cols] = picked.astype(jnp.bfloat16)

    def hid_tile(i, at, width):
        for copy in hid_copy(i, at, width):
            copy.wait()
        cols = pl.ds(at, width)
        gate_pre = jnp.dot(chosen[...], gate_mat[:, cols], preferred_element_type=jnp.float32)
        up_pre = jnp.dot(chosen[...], up_mat[:, cols], preferred_element_type=jnp.float32)
        gated = jnp.minimum(gate_pre, clamp_limit)
        upper = jnp.clip(up_pre, -clamp_limit, clamp_limit)
        value = gated * jax.nn.sigmoid(sig_alpha * gated) * (upper + 1.0)
        hidden[:, cols] = value.astype(jnp.bfloat16)

    @pl.loop(0, hid_tiles)
    def _(i):
        hid_tile(i, pl.multiple_of(i * tile, tile), tile)

    if tail:
        hid_tile(hid_tiles, hid_tiles * tile, tail)

    @pl.loop(0, out_tiles)
    def _(i):
        at = pl.multiple_of(i * tile, tile)
        out_copy(i, at).wait()
        cols = pl.ds(at, tile)
        out = jnp.dot(hidden[...], down_mat[:, cols], preferred_element_type=jnp.float32)
        out = out.astype(jnp.bfloat16)
        for p in range(pairs):
            full = jnp.dot(
                spread[p], out[p * slots : (p + 1) * slots], preferred_element_type=jnp.float32
            )
            full = (full * weight[p]).astype(jnp.bfloat16)
            own_out[p * tok_rows : (p + 1) * tok_rows, cols] = full[:tok_rows]
            other_out[p * tok_rows : (p + 1) * tok_rows, cols] = full[tok_rows:]


def expert_blocks(which, groups, w_gate, w_up, w_down, tok_rows, capacity, experts):
    pairs, pieces = len(groups), len(groups[0]) // 2
    flat = [v for g in groups for v in g]
    feat_width, hid_width = w_gate.shape[1:]
    tokens, slots = 2 * tok_rows, 2 * capacity
    rows = pairs * slots
    shape = jax.ShapeDtypeStruct((pairs * tok_rows, feat_width), jnp.bfloat16)
    vmem = pl.BlockSpec(memory_space=pltpu.VMEM)
    return pl.pallas_call(
        functools.partial(expert_kernel, tok_rows, capacity, experts, pieces, pairs),
        out_shape=(shape, shape),
        in_specs=[pl.BlockSpec(memory_space=pltpu.SMEM)]
        + [vmem] * len(flat)
        + [pl.BlockSpec(memory_space=pltpu.HBM)] * 3,
        out_specs=(vmem, vmem),
        scratch_shapes=[
            pltpu.VMEM((feat_width, hid_width), jnp.bfloat16),
            pltpu.VMEM((feat_width, hid_width), jnp.bfloat16),
            pltpu.VMEM((hid_width, feat_width), jnp.bfloat16),
            pltpu.VMEM((rows, feat_width), jnp.bfloat16),
            pltpu.VMEM((rows, hid_width), jnp.bfloat16),
            pltpu.VMEM((pairs, tokens, 256), jnp.float32),
            pltpu.VMEM((pairs, tokens, slots), jnp.bfloat16),
            pltpu.VMEM((pairs, slots, tokens), jnp.bfloat16),
            pltpu.SemaphoreType.DMA((3, 8)),
        ],
        compiler_params=pltpu.CompilerParams(vmem_limit_bytes=40 * 2**20),
        cost_estimate=pl.CostEstimate(
            flops=6 * rows * feat_width * hid_width,
            bytes_accessed=6 * feat_width * hid_width,
            transcendentals=rows * hid_width,
        ),
    )(which, *flat, w_gate, w_up, w_down)


def add_kernel(*refs):
    total = refs[0][...].astype(jnp.float32)
    for ref in refs[1:-1]:
        total = total + ref[...].astype(jnp.float32)
    refs[-1][...] = total.astype(jnp.bfloat16)


def add_piece(own, returned, piece, rows, arrived):
    width = own.shape[1]
    picked = pl.BlockSpec((rows, width), lambda g: (piece, 0))
    whole = pl.BlockSpec((rows, width), lambda g: (0, 0))
    return pl.pallas_call(
        add_kernel,
        grid=(1,),
        out_shape=jax.ShapeDtypeStruct((rows, width), jnp.bfloat16),
        in_specs=[picked, picked] + [whole] * len(arrived),
        out_specs=whole,
        compiler_params=pltpu.CompilerParams(vmem_limit_bytes=8 * 2**20),
        cost_estimate=pl.CostEstimate(flops=rows * width, bytes_accessed=0, transcendentals=0),
    )(own, returned, *arrived)


def ring_local(tokens, expert_ids, route_weights, norm_gain, w_gate, w_up, w_down):
    ep_count = lax.axis_size("ep")
    tp_count = lax.axis_size("tp")
    experts = ep_count * tp_count
    tok_rows, _ = tokens.shape
    capacity = 2 * tok_rows * expert_ids.shape[1] // experts
    half = ep_count // 2
    order = list(range(0, ep_count, 2)) + list(range(ep_count - 1, 0, -2))
    ahead = [(order[i], order[(i + 1) % ep_count]) for i in range(ep_count)]
    behind = [(b, a) for a, b in ahead]
    swap = [(0, 1), (1, 0)]
    pieces = 2
    rows = tok_rows // pieces
    normed = layer_norm(tokens, norm_gain)
    fits = expert_ids[:, :, None] == jnp.arange(experts, dtype=jnp.int32)
    weights = jnp.sum(jnp.where(fits, route_weights[:, :, None], 0.0), 1)
    high = weights.astype(jnp.bfloat16)
    low = (weights - high.astype(jnp.float32)).astype(jnp.bfloat16)
    lanes = -(-2 * experts // 128) * 128
    gap = jnp.zeros((tok_rows, lanes - 2 * experts), jnp.bfloat16)
    packed = jnp.concatenate([normed, high, low, gap], 1)
    start = [packed[c * rows : (c + 1) * rows] for c in range(pieces)]
    which = (lax.axis_index("ep") * tp_count + lax.axis_index("tp")).astype(jnp.int32).reshape(1)

    def shift(value, pairs):
        return lax.ppermute(value, "ep", pairs)

    def other(value):
        return lax.ppermute(value, "tp", swap)

    held = [[{} for _ in range(half + 1)] for _ in range(2)]
    for direction in range(2):
        held[direction][0] = {c: start[c] for c in range(pieces)}
    for step in range(1, half + 1):
        for c in range(pieces):
            for direction, pairs in ((0, ahead), (1, behind)):
                if step == half and c % 2 != direction:
                    continue
                held[direction][step][c] = shift(held[direction][step - 1][c], pairs)

    sums = [[{} for _ in range(half + 1)] for _ in range(2)]
    for step in range(half + 1):
        if step == 0:
            groups = [[(0, c) for c in range(pieces)]]
        elif step == half:
            groups = [[(c % 2, c) for c in range(pieces)]]
        else:
            groups = [[(d, c) for c in range(pieces)] for d in range(2)]
        values = []
        for g in groups:
            mine = [held[d][step][c] for d, c in g]
            swapped = []
            for (d, c), v in zip(g, mine):
                swapped.append(other(v))
            values.append(mine + swapped)
        own, theirs = expert_blocks(
            which, values, w_gate, w_up, w_down, tok_rows, capacity, experts
        )
        returned = other(theirs)
        for i, (d, c) in enumerate([k for g in groups for k in g]):
            sums[d][step][c] = (own, returned, i, rows)

    arrived = [{}, {}]
    for step in range(half, 0, -1):
        for direction, pairs in ((0, behind), (1, ahead)):
            for c in sorted(sums[direction][step]):
                before = [arrived[direction][c]] if c in arrived[direction] else []
                total = add_piece(*sums[direction][step][c], before)
                arrived[direction][c] = shift(total, pairs)
    done = [
        add_piece(*sums[0][0][c], [arrived[0][c], arrived[1][c]]) for c in range(pieces)
    ]
    return jnp.concatenate(done, 0)


def is_ring(mesh, tok_rows, top_count):
    ep_count, tp_count = mesh.shape["ep"], mesh.shape["tp"]
    capacity = 2 * tok_rows * top_count // (ep_count * tp_count)
    return 2 * capacity >= tok_rows and ep_count % 2 == 0 and ep_count >= 6 and tp_count == 2


def solution(mesh):
    placed = (
        P(("grp", "ep", "tp"), None),
        P(("grp", "ep", "tp"), None),
        P(("grp", "ep", "tp"), None),
        P(),
        P(("ep", "tp"), None, None),
        P(("ep", "tp"), None, None),
        P(("ep", "tp"), None, None),
    )

    def body(tokens, expert_ids, *rest):
        ring = is_ring(mesh, tokens.shape[0], expert_ids.shape[1])
        return (ring_local if ring else local)(tokens, expert_ids, *rest)

    return jax.shard_map(
        body, mesh=mesh, in_specs=placed, out_specs=P(("grp", "ep", "tp"), None), check_vma=False
    )
```

```python
import functools

import jax
import jax.numpy as jnp
from jax import lax
from jax.experimental import pallas as pl
from jax.experimental.pallas import tpu as pltpu
from jax.sharding import PartitionSpec as P


norm_eps = 1e-05
clamp_limit = 7.0
sig_alpha = 1.702


def layer_norm(tokens, norm_gain):
    values = tokens.astype(jnp.float32)
    row_mean = jnp.mean(values, -1, keepdims=True)
    centred = values - row_mean
    row_var = jnp.mean(centred * centred, -1, keepdims=True)
    scaled = centred * lax.rsqrt(row_var + norm_eps) * norm_gain
    return scaled.astype(jnp.bfloat16)


def expert_apply(inputs, gate_mat, up_mat, down_mat):
    gate_pre = jnp.dot(inputs, gate_mat, preferred_element_type=jnp.float32)
    up_pre = jnp.dot(inputs, up_mat, preferred_element_type=jnp.float32)
    gated = jnp.minimum(gate_pre, clamp_limit)
    upper = jnp.clip(up_pre, -clamp_limit, clamp_limit)
    hidden = (gated * jax.nn.sigmoid(sig_alpha * gated) * (upper + 1.0)).astype(jnp.bfloat16)
    return jnp.dot(hidden, down_mat, preferred_element_type=jnp.float32).astype(jnp.bfloat16)


def local(tokens, expert_ids, route_weights, norm_gain, w_gate, w_up, w_down):
    ep_count = lax.axis_size("ep")
    tp_count = lax.axis_size("tp")
    experts = ep_count * tp_count
    tok_rows, feat_width = tokens.shape
    top_count = expert_ids.shape[1]
    capacity = 2 * tok_rows * top_count // experts
    normed = layer_norm(tokens, norm_gain)
    flat_ids = expert_ids.reshape(-1)
    one_hot = (flat_ids[:, None] == jnp.arange(experts, dtype=jnp.int32)[None, :]).astype(jnp.int32)
    slot_index = jnp.sum((jnp.cumsum(one_hot, 0) - one_hot) * one_hot, 1)
    target = flat_ids * capacity + slot_index
    pair_token = jnp.arange(tok_rows * top_count, dtype=jnp.int32) // top_count
    buffer = (
        jnp.zeros((experts * capacity, feat_width), jnp.bfloat16).at[target].set(normed[pair_token])
    )
    buffer = buffer.reshape(experts, capacity, feat_width)
    gate_mat = w_gate[0]
    up_mat = w_up[0]
    down_mat = w_down[0]
    arrived = lax.all_to_all(buffer, ("ep", "tp"), split_axis=0, concat_axis=0, tiled=True)
    flat_rows = arrived.reshape(-1, feat_width)
    returned = lax.all_to_all(
        expert_apply(flat_rows, gate_mat, up_mat, down_mat).reshape(arrived.shape),
        ("ep", "tp"),
        split_axis=0,
        concat_axis=0,
        tiled=True,
    )
    picked = returned.reshape(experts * capacity, feat_width)[target].reshape(
        tok_rows, top_count, feat_width
    )
    combined = jnp.zeros((tok_rows, feat_width), jnp.float32)
    for choice_slot in range(top_count):
        combined = combined + route_weights[:, choice_slot : choice_slot + 1] * picked[
            :, choice_slot
        ].astype(jnp.float32)
    return combined.astype(jnp.bfloat16)


def expert_kernel(tok_rows, capacity, experts, pieces, pairs, *refs):
    number = pairs * 2 * pieces
    which = refs[0]
    blocks = refs[1 : 1 + number]
    gate_mat, up_mat, down_mat, own_out, other_out = refs[1 + number : 6 + number]
    chosen, hidden, weight, spread, gather = refs[6 + number :]
    feat_width, hid_width = gate_mat.shape[1:]
    tile = 256
    hid_tiles, out_tiles = hid_width // tile, feat_width // tile
    tail = hid_width - hid_tiles * tile

    tokens, slots = 2 * tok_rows, 2 * capacity
    row = lax.broadcasted_iota(jnp.int32, (tokens, tokens), 0)
    col = lax.broadcasted_iota(jnp.int32, (tokens, tokens), 1)
    earlier = (col < row) & ((col >= tok_rows) == (row >= tok_rows))
    earlier = jnp.where(earlier, 1.0, 0.0).astype(jnp.bfloat16)
    for p in range(pairs):
        mine = blocks[p * 2 * pieces : (p + 1) * 2 * pieces]
        extra = jnp.concatenate([r[:, feat_width:] for r in mine], 0).astype(jnp.float32)
        lane = lax.broadcasted_iota(jnp.int32, extra.shape, 1)
        wanted = (lane == which[0]) | (lane == which[0] + experts)
        scale = jnp.sum(jnp.where(wanted, extra, 0.0), 1, keepdims=True)
        mask = jnp.broadcast_to(jnp.where(scale > 0.0, 1.0, 0.0), (tokens, slots))
        place = jnp.dot(earlier, mask.astype(jnp.bfloat16), preferred_element_type=jnp.float32)
        line = lax.broadcasted_iota(jnp.int32, (tokens, slots), 0)
        slot = lax.broadcasted_iota(jnp.int32, (tokens, slots), 1)
        target = place.astype(jnp.int32) + jnp.where(line >= tok_rows, capacity, 0)
        one_hot = jnp.where((target == slot) & (mask > 0.0), 1.0, 0.0)
        spread[p] = one_hot.astype(jnp.bfloat16)
        gather[p] = one_hot.T.astype(jnp.bfloat16)
        weight[p] = jnp.broadcast_to(scale, (tokens, tile))

        @pl.loop(0, feat_width // tile)
        def _(i):
            cols = pl.ds(pl.multiple_of(i * tile, tile), tile)
            part = jnp.concatenate([r[:, cols] for r in mine], 0)
            picked = jnp.dot(gather[p], part, preferred_element_type=jnp.float32)
            chosen[p * slots : (p + 1) * slots, cols] = picked.astype(jnp.bfloat16)

    def hid_tile(at, width):
        cols = pl.ds(at, width)
        gate_pre = jnp.dot(chosen[...], gate_mat[0, :, cols], preferred_element_type=jnp.float32)
        up_pre = jnp.dot(chosen[...], up_mat[0, :, cols], preferred_element_type=jnp.float32)
        gated = jnp.minimum(gate_pre, clamp_limit)
        upper = jnp.clip(up_pre, -clamp_limit, clamp_limit)
        value = gated * jax.nn.sigmoid(sig_alpha * gated) * (upper + 1.0)
        hidden[:, cols] = value.astype(jnp.bfloat16)

    @pl.loop(0, hid_tiles)
    def _(i):
        hid_tile(pl.multiple_of(i * tile, tile), tile)

    if tail:
        hid_tile(hid_tiles * tile, tail)

    @pl.loop(0, out_tiles)
    def _(i):
        at = pl.multiple_of(i * tile, tile)
        cols = pl.ds(at, tile)
        out = jnp.dot(hidden[...], down_mat[0, :, cols], preferred_element_type=jnp.float32)
        out = out.astype(jnp.bfloat16)
        for p in range(pairs):
            full = jnp.dot(
                spread[p], out[p * slots : (p + 1) * slots], preferred_element_type=jnp.float32
            )
            full = (full * weight[p]).astype(jnp.bfloat16)
            own_out[p * tok_rows : (p + 1) * tok_rows, cols] = full[:tok_rows]
            other_out[p * tok_rows : (p + 1) * tok_rows, cols] = full[tok_rows:]


def expert_blocks(which, groups, w_gate, w_up, w_down, tok_rows, capacity, experts):
    pairs, pieces = len(groups), len(groups[0]) // 2
    flat = [v for g in groups for v in g]
    feat_width, hid_width = w_gate.shape[1:]
    tokens, slots = 2 * tok_rows, 2 * capacity
    rows = pairs * slots
    shape = jax.ShapeDtypeStruct((pairs * tok_rows, feat_width), jnp.bfloat16)
    vmem = pl.BlockSpec(memory_space=pltpu.VMEM)
    return pl.pallas_call(
        functools.partial(expert_kernel, tok_rows, capacity, experts, pieces, pairs),
        out_shape=(shape, shape),
        in_specs=[pl.BlockSpec(memory_space=pltpu.SMEM)]
        + [vmem] * len(flat)
        + [vmem] * 3,
        out_specs=(vmem, vmem),
        scratch_shapes=[
            pltpu.VMEM((rows, feat_width), jnp.bfloat16),
            pltpu.VMEM((rows, hid_width), jnp.bfloat16),
            pltpu.VMEM((pairs, tokens, 256), jnp.float32),
            pltpu.VMEM((pairs, tokens, slots), jnp.bfloat16),
            pltpu.VMEM((pairs, slots, tokens), jnp.bfloat16),
        ],
        compiler_params=pltpu.CompilerParams(vmem_limit_bytes=26 * 2**20),
        cost_estimate=pl.CostEstimate(
            flops=6 * rows * feat_width * hid_width,
            bytes_accessed=6 * feat_width * hid_width,
            transcendentals=rows * hid_width,
        ),
    )(which, *flat, w_gate, w_up, w_down)


def add_kernel(*refs):
    total = refs[0][...].astype(jnp.float32)
    for ref in refs[1:-1]:
        total = total + ref[...].astype(jnp.float32)
    refs[-1][...] = total.astype(jnp.bfloat16)


def add_piece(own, returned, piece, rows, arrived):
    width = own.shape[1]
    picked = pl.BlockSpec((rows, width), lambda g: (piece, 0))
    whole = pl.BlockSpec((rows, width), lambda g: (0, 0))
    return pl.pallas_call(
        add_kernel,
        grid=(1,),
        out_shape=jax.ShapeDtypeStruct((rows, width), jnp.bfloat16),
        in_specs=[picked, picked] + [whole] * len(arrived),
        out_specs=whole,
        compiler_params=pltpu.CompilerParams(vmem_limit_bytes=8 * 2**20),
        cost_estimate=pl.CostEstimate(flops=rows * width, bytes_accessed=0, transcendentals=0),
    )(own, returned, *arrived)


def ring_local(tokens, expert_ids, route_weights, norm_gain, w_gate, w_up, w_down):
    ep_count = lax.axis_size("ep")
    tp_count = lax.axis_size("tp")
    experts = ep_count * tp_count
    tok_rows, _ = tokens.shape
    capacity = 2 * tok_rows * expert_ids.shape[1] // experts
    half = ep_count // 2
    order = list(range(0, ep_count, 2)) + list(range(ep_count - 1, 0, -2))
    ahead = [(order[i], order[(i + 1) % ep_count]) for i in range(ep_count)]
    behind = [(b, a) for a, b in ahead]
    swap = [(0, 1), (1, 0)]
    pieces = 2
    rows = tok_rows // pieces
    normed = layer_norm(tokens, norm_gain)
    fits = expert_ids[:, :, None] == jnp.arange(experts, dtype=jnp.int32)
    weights = jnp.sum(jnp.where(fits, route_weights[:, :, None], 0.0), 1)
    high = weights.astype(jnp.bfloat16)
    low = (weights - high.astype(jnp.float32)).astype(jnp.bfloat16)
    lanes = -(-2 * experts // 128) * 128
    gap = jnp.zeros((tok_rows, lanes - 2 * experts), jnp.bfloat16)
    packed = jnp.concatenate([normed, high, low, gap], 1)
    start = [packed[c * rows : (c + 1) * rows] for c in range(pieces)]
    which = (lax.axis_index("ep") * tp_count + lax.axis_index("tp")).astype(jnp.int32).reshape(1)

    def shift(value, pairs):
        return lax.ppermute(value, "ep", pairs)

    def other(value):
        return lax.ppermute(value, "tp", swap)

    held = [[{} for _ in range(half + 1)] for _ in range(2)]
    for direction in range(2):
        held[direction][0] = {c: start[c] for c in range(pieces)}
    for step in range(1, half + 1):
        for c in range(pieces):
            for direction, pairs in ((0, ahead), (1, behind)):
                if step == half and c % 2 != direction:
                    continue
                held[direction][step][c] = shift(held[direction][step - 1][c], pairs)

    sums = [[{} for _ in range(half + 1)] for _ in range(2)]
    for step in range(half + 1):
        if step == 0:
            groups = [[(0, c) for c in range(pieces)]]
        elif step == half:
            groups = [[(c % 2, c) for c in range(pieces)]]
        else:
            groups = [[(d, c) for c in range(pieces)] for d in range(2)]
        values = []
        for g in groups:
            mine = [held[d][step][c] for d, c in g]
            swapped = []
            for (d, c), v in zip(g, mine):
                swapped.append(other(v))
            values.append(mine + swapped)
        own, theirs = expert_blocks(
            which, values, w_gate, w_up, w_down, tok_rows, capacity, experts
        )
        returned = other(theirs)
        for i, (d, c) in enumerate([k for g in groups for k in g]):
            sums[d][step][c] = (own, returned, i, rows)

    arrived = [{}, {}]
    for step in range(half, 0, -1):
        for direction, pairs in ((0, behind), (1, ahead)):
            for c in sorted(sums[direction][step]):
                before = [arrived[direction][c]] if c in arrived[direction] else []
                total = add_piece(*sums[direction][step][c], before)
                arrived[direction][c] = shift(total, pairs)
    done = [
        add_piece(*sums[0][0][c], [arrived[0][c], arrived[1][c]]) for c in range(pieces)
    ]
    return jnp.concatenate(done, 0)


def is_ring(mesh, tok_rows, top_count):
    ep_count, tp_count = mesh.shape["ep"], mesh.shape["tp"]
    capacity = 2 * tok_rows * top_count // (ep_count * tp_count)
    return 2 * capacity >= tok_rows and ep_count % 2 == 0 and ep_count >= 6 and tp_count == 2


def solution(mesh):
    placed = (
        P(("grp", "ep", "tp"), None),
        P(("grp", "ep", "tp"), None),
        P(("grp", "ep", "tp"), None),
        P(),
        P(("ep", "tp"), None, None),
        P(("ep", "tp"), None, None),
        P(("ep", "tp"), None, None),
    )

    def body(tokens, expert_ids, *rest):
        ring = is_ring(mesh, tokens.shape[0], expert_ids.shape[1])
        return (ring_local if ring else local)(tokens, expert_ids, *rest)

    return jax.shard_map(
        body, mesh=mesh, in_specs=placed, out_specs=P(("grp", "ep", "tp"), None), check_vma=False
    )
```
